32 devices in a mesh: rep: 2 (over x), fs: 8 (over z, y), tp: 2 (over core).
Axes of the slice: x: 2, y: 2, z: 4, core: 2. Of those that a mesh axis runs over, the one named last changes fastest.
Arguments:
- tokens: bfloat16 [8192, 2048], P(('rep', 'fs'), 'tp'), may hold values from -6 to 6
- mix_gain: float32 [2048], replicated, may hold values from 0.1 to 1.9
- lru_input: float32 [2048, 2048], P('fs', 'tp'), may hold values from -0.125 to 0.125
- lru_gate: float32 [2048, 2048], P('fs', 'tp'), may hold values from -0.125 to 0.125
- lru_input_scale: float32 [2048], P('tp'), may hold values from 0.5 to 2
- lru_gate_scale: float32 [2048], P('tp'), may hold values from 0.5 to 2
- conv_weight: float32 [4, 2048], P(None, 'tp'), may hold values from -3 to 3
- recur_gate: float32 [32, 64, 64], P('tp'), may hold values from -0.75 to 0.75
- input_gate: float32 [32, 64, 64], P('tp'), may hold values from -0.75 to 0.75
- decay_rate: float32 [2048], P('tp'), may hold values from 3.5 to 9
- extra_decay: float32 [8192], P(('rep', 'fs')), may hold values from 0.0003 to 2.1
- lru_output: float32 [2048, 2048], P('tp', 'fs'), may hold values from -0.125 to 0.125
- lru_output_scale: float32 [2048], replicated, may hold values from 0.5 to 2
- ffn_gain: float32 [2048], replicated, may hold values from 0.1 to 1.9
- ffn_gate: float32 [2048, 2816], P('fs', 'tp'), may hold values from -0.125 to 0.125
- ffn_up: float32 [2048, 2816], P('fs', 'tp'), may hold values from -0.125 to 0.125
- ffn_gate_scale: float32 [2816], P('tp'), may hold values from 0.5 to 2
- ffn_up_scale: float32 [2816], P('tp'), may hold values from 0.5 to 2
- ffn_down: float32 [2816, 2048], P('tp', 'fs'), may hold values from -0.109375 to 0.109375
- ffn_down_scale: float32 [2048], replicated, may hold values from 0.5 to 2
Outputs:
- layer_out: bfloat16 [8192, 2048], P(('rep', 'fs'), 'tp')
The draws below stay inside these ranges and needn't reach their ends.
All inputs are finite; a program needn't handle non-finite values.
Results may differ from the reference program's by a relative error of at most 0.02.
Values may be sent and summed in bfloat16 or wider, within the bound.
A program may use at most 192 MiB of HBM per device.

```python
import math
import jax
import jax.numpy as jnp
from jax import lax

D = 2048
FF = 2816
BDIM = 64
LRU_BLOCKS = 32
CONV = 4
TOK_DEV = 512
LRU = 2048
SEQS = 16
TOKENS = 8192
N_TP = 2


def draw_decay_rate(key, part):
    first, second, third = jax.random.split(jax.random.fold_in(key, 11), 3)
    share = 0.5
    slow = jax.random.uniform(first, (LRU,), jnp.float32) < share
    slow_value = jax.random.uniform(second, (LRU,), jnp.float32, 8.0, 9.0)
    fast_value = jax.random.uniform(third, (LRU,), jnp.float32, 3.5, 4.5)
    return jnp.where(slow, slow_value, fast_value)


def draw_extra_decay(key, part):
    first, second, third = jax.random.split(jax.random.fold_in(key, 23), 3)
    base = jnp.exp(jax.random.uniform(first, (SEQS, 1), jnp.float32, jnp.log(0.0003), jnp.log(0.0009)))
    spots = jax.random.randint(second, (SEQS, 3), 0, TOK_DEV)
    where = jnp.arange(TOK_DEV, dtype=jnp.int32)
    hits = jnp.sum((where[None, None, :] == spots[:, :, None]).astype(jnp.float32), axis=1)
    sizes = jax.random.uniform(third, (SEQS, TOK_DEV), jnp.float32, 0.22, 0.69)
    return (base + hits * sizes).reshape(TOKENS)


def block_scale(rng, shape, cuts, smallest, top_value):
    def one(position, shards_of):
        draws = jax.random.uniform(jax.random.fold_in(jax.random.fold_in(rng, 6), position), (shards_of,), jnp.float32, smallest / len(cuts), top_value / len(cuts))
        return jnp.repeat(jnp.exp(draws), shape[position] // shards_of).reshape((-1,) + (1,) * (len(shape) - position - 1))

    loudness = one(*cuts[0])
    for cut in cuts[1:]:
        loudness = loudness * one(*cut)
    return loudness


def gaussian(rng, shape, scale, most, cuts=(), kind=jnp.bfloat16):
    entries = jax.random.normal(rng, shape, jnp.float32) * scale
    if len(cuts) > 0:
        entries = block_scale(rng, shape, cuts, -0.22, 0.18) * entries
    return jnp.clip(entries, min=-most, max=most).astype(kind)


def setup_inputs(seed: int = 0) -> dict:
    key_of = jax.random.split(jax.random.key(seed), 21)
    tokens = gaussian(key_of[0], (TOKENS, D), 1.0, 6.0, ((0, 16), (1, 2)))
    mix_gain = jnp.clip(1.0 + 0.18 * jax.random.normal(key_of[1], (D,), jnp.float32), 0.1, 1.9)
    lru_input = gaussian(key_of[2], (D, LRU), D ** -0.5, 0.125, ((0, 8), (1, 2)), jnp.float32)
    lru_gate = gaussian(key_of[3], (D, LRU), D ** -0.5, 0.125, ((0, 8), (1, 2)), jnp.float32)
    lru_input_scale = jnp.clip(jnp.exp(math.log(2.0) - 1.3862944 * jax.random.uniform(key_of[4], (LRU,), jnp.float32) ** block_scale(key_of[4], (LRU,), ((0, 2),), -0.2, 0.2)), 0.5, 2.0)
    lru_gate_scale = jnp.clip(jnp.exp(math.log(2.0) - 1.3862944 * jax.random.uniform(key_of[5], (LRU,), jnp.float32) ** block_scale(key_of[5], (LRU,), ((0, 2),), -0.2, 0.2)), 0.5, 2.0)
    conv_weight = gaussian(key_of[6], (CONV, LRU), 0.5, 3.0, ((1, 2),), jnp.float32)
    recur_gate = gaussian(key_of[7], (LRU_BLOCKS, BDIM, BDIM), BDIM ** -0.5, 0.75, ((0, 2),), jnp.float32)
    input_gate = gaussian(key_of[8], (LRU_BLOCKS, BDIM, BDIM), BDIM ** -0.5, 0.75, ((0, 2),), jnp.float32)
    decay_rate = draw_decay_rate(jax.random.fold_in(key_of[20], 71), 0)
    extra_decay = draw_extra_decay(jax.random.fold_in(key_of[20], 71), 0)
    lru_output = gaussian(key_of[11], (LRU, D), LRU ** -0.5, 0.125, ((0, 2), (1, 8)), jnp.float32)
    lru_output_scale = jnp.clip(jnp.exp(jax.random.uniform(key_of[12], (D,), jnp.float32, math.log(0.5), math.log(2.0))), 0.5, 2.0)
    ffn_gain = jnp.clip(1.0 + 0.18 * jax.random.normal(key_of[13], (D,), jnp.float32), 0.1, 1.9)
    ffn_gate = gaussian(key_of[14], (D, FF), D ** -0.5, 0.125, ((0, 8), (1, 2)), jnp.float32)
    ffn_up = gaussian(key_of[15], (D, FF), D ** -0.5, 0.125, ((0, 8), (1, 2)), jnp.float32)
    ffn_gate_scale = jnp.clip(jnp.exp(math.log(2.0) - 1.3862944 * jax.random.uniform(key_of[16], (FF,), jnp.float32) ** block_scale(key_of[16], (FF,), ((0, 2),), -0.2, 0.2)), 0.5, 2.0)
    ffn_up_scale = jnp.clip(jnp.exp(math.log(2.0) - 1.3862944 * jax.random.uniform(key_of[17], (FF,), jnp.float32) ** block_scale(key_of[17], (FF,), ((0, 2),), -0.2, 0.2)), 0.5, 2.0)
    ffn_down = gaussian(key_of[18], (FF, D), FF ** -0.5, 0.109375, ((0, 2), (1, 8)), jnp.float32)
    ffn_down_scale = jnp.clip(jnp.exp(jax.random.uniform(key_of[19], (D,), jnp.float32, math.log(0.5), math.log(2.0))), 0.5, 2.0)
    return dict(tokens=tokens, mix_gain=mix_gain, lru_input=lru_input, lru_gate=lru_gate, lru_input_scale=lru_input_scale, lru_gate_scale=lru_gate_scale, conv_weight=conv_weight, recur_gate=recur_gate, input_gate=input_gate, decay_rate=decay_rate, extra_decay=extra_decay, lru_output=lru_output, lru_output_scale=lru_output_scale, ffn_gain=ffn_gain, ffn_gate=ffn_gate, ffn_up=ffn_up, ffn_gate_scale=ffn_gate_scale, ffn_up_scale=ffn_up_scale, ffn_down=ffn_down, ffn_down_scale=ffn_down_scale)


EPS = 1e-06
RATE = 8.0

def rms_rows(rows, gain):
    values = rows.astype(jnp.float32)
    scale = lax.rsqrt(lax.optimization_barrier(jnp.mean(values * values, axis=-1, keepdims=True)) + EPS)
    return (values * scale * gain).astype(jnp.bfloat16)

def block_sum(acts, weight, blocks):
    width = acts.shape[1] // blocks
    total = jnp.zeros((acts.shape[0], weight.shape[1]), jnp.float32)
    for block in range(blocks):
        part = jnp.dot(acts[:, block * width:(block + 1) * width], weight[block * width:(block + 1) * width].astype(jnp.bfloat16), preferred_element_type=jnp.float32).astype(jnp.bfloat16)
        part = lax.optimization_barrier(part)
        total = total + part.astype(jnp.float32)
    return total

def combine(left, right):
    return (left[0] * right[0], right[0] * left[1] + right[1])

def recurrence(branch_in, branch_gate, conv_weight, recur_gate, input_gate, decay_rate, extra):
    length = branch_in.shape[0]
    taps = conv_weight.shape[0]
    values = branch_in.astype(jnp.float32)
    padded = jnp.pad(values, ((taps - 1, 0), (0, 0)))
    conv = jnp.zeros_like(values)
    for tap in range(taps):
        conv = conv + conv_weight[tap] * padded[tap:tap + length]
    nblocks, bdim = (recur_gate.shape[0], recur_gate.shape[1])
    grouped = conv.reshape(length, nblocks, bdim)
    recur = jax.nn.sigmoid(jnp.einsum('sni,nij->snj', grouped, recur_gate, precision=lax.Precision.HIGHEST).reshape(length, -1))
    ingate = jax.nn.sigmoid(jnp.einsum('sni,nij->snj', grouped, input_gate, precision=lax.Precision.HIGHEST).reshape(length, -1))
    log_rate = -RATE * jax.nn.softplus(-decay_rate) * recur - extra[:, None]
    factor = jnp.exp(log_rate)
    drive = jnp.sqrt(-jnp.expm1(2.0 * log_rate)) * (ingate * conv)
    state = lax.associative_scan(combine, (factor, drive), axis=0)[1]
    gelu_gate = jax.nn.gelu(branch_gate.astype(jnp.float32), approximate=True)
    return (state * gelu_gate).astype(jnp.bfloat16)

def reference(tokens, mix_gain, lru_input, lru_gate, lru_input_scale, lru_gate_scale, conv_weight, recur_gate, input_gate, decay_rate, extra_decay, lru_output, lru_output_scale, ffn_gain, ffn_gate, ffn_up, ffn_gate_scale, ffn_up_scale, ffn_down, ffn_down_scale):
    normed = rms_rows(tokens, mix_gain)
    branch_in = (jnp.dot(normed, lru_input.astype(jnp.bfloat16), preferred_element_type=jnp.float32) * lru_input_scale).astype(jnp.bfloat16)
    branch_gate = (jnp.dot(normed, lru_gate.astype(jnp.bfloat16), preferred_element_type=jnp.float32) * lru_gate_scale).astype(jnp.bfloat16)
    width = branch_in.shape[1]
    gated = jax.vmap(recurrence, in_axes=(0, 0, None, None, None, None, 0))(branch_in.reshape(SEQS, TOK_DEV, width), branch_gate.reshape(SEQS, TOK_DEV, width), conv_weight, recur_gate, input_gate, decay_rate, extra_decay.reshape(SEQS, TOK_DEV))
    gated = gated.reshape(TOKENS, width)
    mixed = (tokens.astype(jnp.float32) + block_sum(gated, lru_output, N_TP) * lru_output_scale).astype(jnp.bfloat16)
    normed2 = rms_rows(mixed, ffn_gain)
    gate_pre = jnp.dot(normed2, ffn_gate.astype(jnp.bfloat16), preferred_element_type=jnp.float32) * ffn_gate_scale
    up_pre = jnp.dot(normed2, ffn_up.astype(jnp.bfloat16), preferred_element_type=jnp.float32) * ffn_up_scale
    hidden = (jax.nn.silu(gate_pre) * up_pre).astype(jnp.bfloat16)
    total = block_sum(hidden, ffn_down, N_TP)
    return (mixed.astype(jnp.float32) + total * ffn_down_scale).astype(jnp.bfloat16)
```

```python
import jax
import jax.numpy as jnp
from jax import lax
from jax.experimental import pallas as pl
from jax.experimental.pallas import tpu as pltpu
from jax.sharding import PartitionSpec as P

EPS = 1e-06
RATE = 8.0
LANES = 128


def swap(value, axis):
    return lax.ppermute(value, axis, [(0, 1), (1, 0)])


def sigmoid(v):
    return 1.0 / (1.0 + jnp.exp(-v))


def rec_kernel(in_ref, gate_ref, conv_ref, map_ref, rate_ref, extra_ref, out_ref):
    length = in_ref.shape[0]
    taps = conv_ref.shape[0]
    values = in_ref[...].astype(jnp.float32)
    row = lax.broadcasted_iota(jnp.int32, values.shape, 0)
    conv = conv_ref[taps - 1 : taps, :] * values
    for back in range(1, taps):
        moved = jnp.where(row >= back, pltpu.roll(values, back, 0), 0.0)
        conv = conv + conv_ref[taps - 1 - back : taps - back, :] * moved
    mapped = jnp.dot(
        conv, map_ref[0], preferred_element_type=jnp.float32, precision=lax.Precision.HIGHEST
    )
    recur = sigmoid(mapped[:, :LANES])
    ingate = sigmoid(mapped[:, LANES:])
    log_rate = rate_ref[...] * recur - extra_ref[...]
    a = jnp.exp(log_rate)
    u = -2.0 * log_rate
    series = u * (1 - u / 2 * (1 - u / 3 * (1 - u / 4 * (1 - u / 5 * (1 - u / 6)))))
    b = jnp.sqrt(jnp.where(u < 0.25, series, 1.0 - jnp.exp(-u))) * (ingate * conv)
    inner = row % 8
    for s in (1, 2, 4):
        keep = inner >= s
        b = jnp.where(keep, a * pltpu.roll(b, s, 0) + b, b)
        a = jnp.where(keep, a * pltpu.roll(a, s, 0), a)
    s = 1
    groups = length // 8
    last_a = a.reshape(groups, 8, LANES)
    last_b = b.reshape(groups, 8, LANES)
    ca = jnp.broadcast_to(last_a[:, 7:8, :], last_a.shape).reshape(length, LANES)
    cb = jnp.broadcast_to(last_b[:, 7:8, :], last_b.shape).reshape(length, LANES)
    s = 8
    while s < length:
        cb_new = ca[s:] * cb[:-s] + cb[s:]
        ca_new = ca[s:] * ca[:-s]
        cb = jnp.concatenate([cb[:s], cb_new], axis=0)
        ca = jnp.concatenate([ca[:s], ca_new], axis=0)
        s *= 2
    state = jnp.concatenate([b[:8], a[8:] * cb[:-8] + b[8:]], axis=0)
    g = gate_ref[...].astype(jnp.float32)
    gelu = 0.5 * g * (1.0 + jnp.tanh(0.7978845608028654 * (g + 0.044715 * g * g * g)))
    out_ref[...] = (state * gelu).astype(out_ref.dtype)


def recurrence(branch_in, branch_gate, conv_weight, maps, rate, extra):
    length, width = branch_in.shape
    taps = conv_weight.shape[0]
    tile = lambda rows: pl.BlockSpec((rows, LANES), lambda i: (0, i))
    return pl.pallas_call(
        rec_kernel,
        grid=(width // LANES,),
        in_specs=[
            tile(length),
            tile(length),
            tile(taps),
            pl.BlockSpec((1, LANES, 2 * LANES), lambda i: (i, 0, 0)),
            tile(1),
            pl.BlockSpec((length, 1), lambda i: (0, 0)),
        ],
        out_specs=tile(length),
        out_shape=jax.ShapeDtypeStruct((length, width), jnp.bfloat16),
        cost_estimate=pl.CostEstimate(
            flops=length * width * 16000, bytes_accessed=length * width * 6, transcendentals=0
        ),
        name="recur",
    )(branch_in, branch_gate, conv_weight, maps, rate, extra)


def local(mesh_fs, *args):
    (
        tokens,
        mix_gain,
        lru_input,
        lru_gate,
        lru_input_scale,
        lru_gate_scale,
        conv_weight,
        recur_gate,
        input_gate,
        decay_rate,
        extra_decay,
        lru_output,
        lru_output_scale,
        ffn_gain,
        ffn_gate,
        ffn_up,
        ffn_gate_scale,
        ffn_up_scale,
        ffn_down,
        ffn_down_scale,
    ) = args
    ny = 2 if mesh_fs % 2 == 0 else 1
    nz = mesh_fs // ny
    fs = lax.axis_index("fs")
    z, y = fs // ny, fs % ny
    rep = lax.axis_index("rep")
    tp = lax.axis_index("tp")
    columns = tokens.shape[1]
    bf16, f32 = jnp.bfloat16, jnp.float32

    def half(v, axis):
        size = v.shape[axis] // 2
        return lax.dynamic_slice_in_dim(v, rep * size, size, axis)

    def ring(v, dz, dy):
        pairs = [
            (a * ny + b, ((a + dz) % nz) * ny + (b + dy) % ny)
            for a in range(nz)
            for b in range(ny)
        ]
        return lax.ppermute(v, "fs", pairs)

    def gather(piece, axis):
        size = piece.shape[axis]
        shape = list(piece.shape)
        shape[axis] = size * mesh_fs
        whole = jnp.zeros(shape, piece.dtype)
        firsts = [piece if dz == 0 else ring(piece, dz, 0) for dz in range(nz)]
        for dz in range(nz):
            src_z = (z - dz + nz) % nz
            for dy in range(ny):
                part = firsts[dz] if dy == 0 else ring(firsts[dz], 0, dy)
                src = src_z * ny + (y - dy + ny) % ny
                whole = lax.dynamic_update_slice_in_dim(whole, part, src * size, axis)
        return whole

    def pair_piece(first, second):
        return jnp.concatenate([half(first, 1), half(second, 1)], axis=1).astype(bf16)

    other_half = swap(tokens, "tp")
    pair_tokens = swap(tokens, "rep")
    pair_other = swap(pair_tokens, "tp")
    pair_extra = swap(extra_decay, "rep")

    mix_piece = pair_piece(lru_input, lru_gate)
    out_piece = half(lru_output, 0).astype(bf16)
    ffn_piece = pair_piece(ffn_gate, ffn_up)
    down_piece = half(ffn_down, 0).astype(bf16)
    mix_w = gather(mix_piece, 0)
    out_w = gather(out_piece, 1)
    ffn_w = gather(ffn_piece, 0)
    down_w = gather(down_piece, 1)

    def normed(own, other, gain):
        low = jnp.where(tp == 0, own, other).astype(f32)
        high = jnp.where(tp == 0, other, own).astype(f32)
        total = jnp.sum(low * low, axis=-1, keepdims=True) + jnp.sum(
            high * high, axis=-1, keepdims=True
        )
        scale = lax.rsqrt(total / (2 * columns) + EPS)
        return jnp.concatenate(
            [
                (low * scale * gain[:columns]).astype(bf16),
                (high * scale * gain[columns:]).astype(bf16),
            ],
            axis=1,
        )

    def dot(left, right):
        return jnp.dot(left, right, preferred_element_type=f32)

    nblocks, bdim = half(recur_gate, 0).shape[:2]
    per = LANES // bdim
    eye = jnp.eye(per, dtype=f32)

    def block_diag(blocks):
        grouped = half(blocks, 0).reshape(nblocks // per, per, bdim, bdim)
        return jnp.einsum("gpij,pq->gpiqj", grouped, eye, precision="highest").reshape(
            nblocks // per, LANES, LANES
        )

    maps = jnp.concatenate([block_diag(recur_gate), block_diag(input_gate)], axis=2)
    rate = (-RATE * jax.nn.softplus(-half(decay_rate, 0)))[None, :]
    taps = half(conv_weight, 1)
    mix_scale = jnp.concatenate([half(lru_input_scale, 0), half(lru_gate_scale, 0)])
    ffn_scale = jnp.concatenate([half(ffn_gate_scale, 0), half(ffn_up_scale, 0)])

    def mixer(own, other, extra):
        branches = (dot(normed(own, other, mix_gain), mix_w) * mix_scale).astype(bf16)
        width = branches.shape[1] // 2
        gated = recurrence(
            branches[:, :width], branches[:, width:], taps, maps, rate, extra[:, None]
        )
        return dot(gated, out_w)

    def core_sum(terms):
        mine = lax.dynamic_slice_in_dim(terms, tp * columns, columns, 1)
        theirs = lax.dynamic_slice_in_dim(terms, (1 - tp) * columns, columns, 1).astype(bf16)
        return mine + swap(theirs, "tp").astype(f32)

    def reduce_pair(make, theirs, ours):
        sent = swap(core_sum(make(*theirs)).astype(bf16), "rep")
        return core_sum(make(*ours)) + sent.astype(f32)

    def own(v):
        return lax.dynamic_slice_in_dim(v, tp * columns, columns)

    total = reduce_pair(
        mixer, (pair_tokens, pair_other, pair_extra), (tokens, other_half, extra_decay)
    )
    mixed = (tokens.astype(f32) + total * own(lru_output_scale)).astype(bf16)

    mixed_other = swap(mixed, "tp")
    pair_mixed = swap(mixed, "rep")
    pair_mixed_other = swap(pair_mixed, "tp")

    def feed(own_part, other_part):
        both = dot(normed(own_part, other_part, ffn_gain), ffn_w) * ffn_scale
        width = both.shape[1] // 2
        hidden = (jax.nn.silu(both[:, :width]) * both[:, width:]).astype(bf16)
        return dot(hidden, down_w)

    summed = reduce_pair(feed, (pair_mixed, pair_mixed_other), (mixed, mixed_other))
    return (mixed.astype(f32) + summed * own(ffn_down_scale)).astype(bf16)


def solution(mesh):
    in_specs = (
        P(("rep", "fs"), "tp"),
        P(),
        P("fs", "tp"),
        P("fs", "tp"),
        P("tp"),
        P("tp"),
        P(None, "tp"),
        P("tp", None, None),
        P("tp", None, None),
        P("tp"),
        P(("rep", "fs")),
        P("tp", "fs"),
        P(),
        P(),
        P("fs", "tp"),
        P("fs", "tp"),
        P("tp"),
        P("tp"),
        P("tp", "fs"),
        P(),
    )
    out_specs = P(("rep", "fs"), "tp")
    mesh_fs = mesh.shape["fs"]
    return jax.shard_map(
        lambda *args: local(mesh_fs, *args),
        mesh=mesh,
        in_specs=in_specs,
        out_specs=out_specs,
        check_vma=False,
    )
```

```python
import jax
import jax.numpy as jnp
from jax import lax
from jax.experimental import pallas as pl
from jax.experimental.pallas import tpu as pltpu
from jax.sharding import PartitionSpec as P

EPS = 1e-06
RATE = 8.0
AHEAD = 2
LANES = 128


def swap(value, axis):
    return lax.ppermute(value, axis, [(0, 1), (1, 0)])


def sigmoid(v):
    return 1.0 / (1.0 + jnp.exp(-v))


def rec_kernel(in_ref, gate_ref, conv_ref, map_ref, rate_ref, extra_ref, out_ref):
    length = in_ref.shape[0]
    taps = conv_ref.shape[0]
    values = in_ref[...].astype(jnp.float32)
    row = lax.broadcasted_iota(jnp.int32, values.shape, 0)
    conv = conv_ref[taps - 1 : taps, :] * values
    for back in range(1, taps):
        moved = jnp.where(row >= back, pltpu.roll(values, back, 0), 0.0)
        conv = conv + conv_ref[taps - 1 - back : taps - back, :] * moved
    mapped = jnp.dot(
        conv, map_ref[0], preferred_element_type=jnp.float32, precision=lax.Precision.HIGHEST
    )
    recur = sigmoid(mapped[:, :LANES])
    ingate = sigmoid(mapped[:, LANES:])
    log_rate = rate_ref[...] * recur - extra_ref[...]
    a = jnp.exp(log_rate)
    u = -2.0 * log_rate
    series = u * (1 - u / 2 * (1 - u / 3 * (1 - u / 4 * (1 - u / 5 * (1 - u / 6)))))
    b = jnp.sqrt(jnp.where(u < 0.25, series, 1.0 - jnp.exp(-u))) * (ingate * conv)
    inner = row % 8
    for s in (1, 2, 4):
        keep = inner >= s
        b = jnp.where(keep, a * pltpu.roll(b, s, 0) + b, b)
        a = jnp.where(keep, a * pltpu.roll(a, s, 0), a)
    s = 1
    groups = length // 8
    last_a = a.reshape(groups, 8, LANES)
    last_b = b.reshape(groups, 8, LANES)
    ca = jnp.broadcast_to(last_a[:, 7:8, :], last_a.shape).reshape(length, LANES)
    cb = jnp.broadcast_to(last_b[:, 7:8, :], last_b.shape).reshape(length, LANES)
    s = 8
    while s < length:
        cb_new = ca[s:] * cb[:-s] + cb[s:]
        ca_new = ca[s:] * ca[:-s]
        cb = jnp.concatenate([cb[:s], cb_new], axis=0)
        ca = jnp.concatenate([ca[:s], ca_new], axis=0)
        s *= 2
    state = jnp.concatenate([b[:8], a[8:] * cb[:-8] + b[8:]], axis=0)
    g = gate_ref[...].astype(jnp.float32)
    gelu = 0.5 * g * (1.0 + jnp.tanh(0.7978845608028654 * (g + 0.044715 * g * g * g)))
    out_ref[...] = (state * gelu).astype(out_ref.dtype)


def recurrence(branch_in, branch_gate, conv_weight, maps, rate, extra):
    length, width = branch_in.shape
    taps = conv_weight.shape[0]
    tile = lambda rows: pl.BlockSpec((rows, LANES), lambda i: (0, i))
    return pl.pallas_call(
        rec_kernel,
        grid=(width // LANES,),
        in_specs=[
            tile(length),
            tile(length),
            tile(taps),
            pl.BlockSpec((1, LANES, 2 * LANES), lambda i: (i, 0, 0)),
            tile(1),
            pl.BlockSpec((length, 1), lambda i: (0, 0)),
        ],
        out_specs=tile(length),
        out_shape=jax.ShapeDtypeStruct((length, width), jnp.bfloat16),
        cost_estimate=pl.CostEstimate(
            flops=length * width * 16000, bytes_accessed=length * width * 6, transcendentals=0
        ),
        name="recur",
    )(branch_in, branch_gate, conv_weight, maps, rate, extra)


def local(mesh_fs, *args):
    (
        tokens,
        mix_gain,
        lru_input,
        lru_gate,
        lru_input_scale,
        lru_gate_scale,
        conv_weight,
        recur_gate,
        input_gate,
        decay_rate,
        extra_decay,
        lru_output,
        lru_output_scale,
        ffn_gain,
        ffn_gate,
        ffn_up,
        ffn_gate_scale,
        ffn_up_scale,
        ffn_down,
        ffn_down_scale,
    ) = args
    ny = 2 if mesh_fs % 2 == 0 else 1
    nz = mesh_fs // ny
    fs = lax.axis_index("fs")
    z, y = fs // ny, fs % ny
    rep = lax.axis_index("rep")
    tp = lax.axis_index("tp")
    columns = tokens.shape[1]
    bf16, f32 = jnp.bfloat16, jnp.float32

    def half(v, axis):
        size = v.shape[axis] // 2
        return lax.dynamic_slice_in_dim(v, rep * size, size, axis)

    def ring(v, dz, dy):
        pairs = [
            (a * ny + b, ((a + dz) % nz) * ny + (b + dy) % ny)
            for a in range(nz)
            for b in range(ny)
        ]
        return lax.ppermute(v, "fs", pairs)

    chains = {}

    def send(v, dz, dy):
        chain = chains.setdefault((dz, dy), [])
        if len(chain) >= AHEAD:
            v, _ = lax.optimization_barrier((v, chain[-AHEAD]))
        got = ring(v, dz, dy)
        chain.append(got)
        return got

    def swap_y(parts):
        if ny == 1:
            return []
        return [(send(v, 0, 1), src_z, 1 - yy, at) for v, src_z, yy, at in parts]

    def ring_z(parts):
        got = list(parts)
        right, left = list(parts), list(parts)
        for step in range(1, nz // 2):
            right = [(send(v, 1, 0), dz + 1, yy, at) for v, dz, yy, at in right]
            left = [(send(v, -1, 0), dz - 1, yy, at) for v, dz, yy, at in left]
            got += right + left
        if nz > 1:
            for v, dz, yy, at in right:
                got.append((send(v[: v.shape[0] // 2], 1, 0), dz + 1, yy, at))
            for v, dz, yy, at in left:
                cut = v.shape[0] // 2
                got.append((send(v[cut:], -1, 0), dz - 1, yy, at + cut))
        return got

    def place(parts, shape, axis):
        whole = jnp.zeros([n * (mesh_fs if i == axis else 1) for i, n in enumerate(shape)], bf16)
        for v, dz, yy, at in parts:
            src = ((z - dz + nz) % nz) * ny + (y + yy) % ny
            start = [0, 0]
            start[axis] = src * shape[axis]
            start[0] = start[0] + at
            whole = lax.dynamic_update_slice(whole, v, start)
        return whole

    def pair_piece(first, second):
        return jnp.concatenate([half(first, 1), half(second, 1)], axis=1).astype(bf16)

    other_half = swap(tokens, "tp")
    pair_tokens = swap(tokens, "rep")
    pair_other = swap(pair_tokens, "tp")
    pair_extra = swap(extra_decay, "rep")

    mix_piece = pair_piece(lru_input, lru_gate)
    out_piece = half(lru_output, 0).astype(bf16)
    ffn_piece = pair_piece(ffn_gate, ffn_up)
    down_piece = half(ffn_down, 0).astype(bf16)
    mix_own = [(mix_piece, 0, 0, 0)]
    mix_parts = ring_z(mix_own + swap_y(mix_own))
    mix_w = place(mix_parts, mix_piece.shape, 0)
    later = []
    for piece, axis in ((out_piece, 1), (ffn_piece, 0), (down_piece, 1)):
        parts = ring_z([(piece, 0, 0, 0)])
        later.append(place(parts + swap_y(parts), piece.shape, axis))
    out_w, ffn_w, down_w = later

    def normed(own, other, gain):
        low = jnp.where(tp == 0, own, other).astype(f32)
        high = jnp.where(tp == 0, other, own).astype(f32)
        total = jnp.sum(low * low, axis=-1, keepdims=True) + jnp.sum(
            high * high, axis=-1, keepdims=True
        )
        scale = lax.rsqrt(total / (2 * columns) + EPS)
        return jnp.concatenate(
            [
                (low * scale * gain[:columns]).astype(bf16),
                (high * scale * gain[columns:]).astype(bf16),
            ],
            axis=1,
        )

    def dot(left, right):
        return jnp.dot(left, right, preferred_element_type=f32)

    nblocks, bdim = half(recur_gate, 0).shape[:2]
    per = LANES // bdim
    eye = jnp.eye(per, dtype=f32)

    def block_diag(blocks):
        grouped = half(blocks, 0).reshape(nblocks // per, per, bdim, bdim)
        return jnp.einsum("gpij,pq->gpiqj", grouped, eye, precision="highest").reshape(
            nblocks // per, LANES, LANES
        )

    maps = jnp.concatenate([block_diag(recur_gate), block_diag(input_gate)], axis=2)
    rate = (-RATE * jax.nn.softplus(-half(decay_rate, 0)))[None, :]
    taps = half(conv_weight, 1)
    mix_scale = jnp.concatenate([half(lru_input_scale, 0), half(lru_gate_scale, 0)])
    ffn_scale = jnp.concatenate([half(ffn_gate_scale, 0), half(ffn_up_scale, 0)])

    def mixer(own, other, extra):
        branches = (dot(normed(own, other, mix_gain), mix_w) * mix_scale).astype(bf16)
        width = branches.shape[1] // 2
        gated = recurrence(
            branches[:, :width], branches[:, width:], taps, maps, rate, extra[:, None]
        )
        return dot(gated, out_w)

    def core_sum(terms):
        mine = lax.dynamic_slice_in_dim(terms, tp * columns, columns, 1)
        theirs = lax.dynamic_slice_in_dim(terms, (1 - tp) * columns, columns, 1).astype(bf16)
        return mine + swap(theirs, "tp").astype(f32)

    def reduce_pair(make, theirs, ours):
        sent = swap(core_sum(make(*theirs)).astype(bf16), "rep")
        return core_sum(make(*ours)) + sent.astype(f32)

    def own(v):
        return lax.dynamic_slice_in_dim(v, tp * columns, columns)

    total = reduce_pair(
        mixer, (pair_tokens, pair_other, pair_extra), (tokens, other_half, extra_decay)
    )
    mixed = (tokens.astype(f32) + total * own(lru_output_scale)).astype(bf16)

    mixed_other = swap(mixed, "tp")
    pair_mixed = swap(mixed, "rep")
    pair_mixed_other = swap(pair_mixed, "tp")

    def feed(own_part, other_part):
        both = dot(normed(own_part, other_part, ffn_gain), ffn_w) * ffn_scale
        width = both.shape[1] // 2
        hidden = (jax.nn.silu(both[:, :width]) * both[:, width:]).astype(bf16)
        return dot(hidden, down_w)

    summed = reduce_pair(feed, (pair_mixed, pair_mixed_other), (mixed, mixed_other))
    return (mixed.astype(f32) + summed * own(ffn_down_scale)).astype(bf16)


def solution(mesh):
    in_specs = (
        P(("rep", "fs"), "tp"),
        P(),
        P("fs", "tp"),
        P("fs", "tp"),
        P("tp"),
        P("tp"),
        P(None, "tp"),
        P("tp", None, None),
        P("tp", None, None),
        P("tp"),
        P(("rep", "fs")),
        P("tp", "fs"),
        P(),
        P(),
        P("fs", "tp"),
        P("fs", "tp"),
        P("tp"),
        P("tp"),
        P("tp", "fs"),
        P(),
    )
    out_specs = P(("rep", "fs"), "tp")
    mesh_fs = mesh.shape["fs"]
    return jax.shard_map(
        lambda *args: local(mesh_fs, *args),
        mesh=mesh,
        in_specs=in_specs,
        out_specs=out_specs,
        check_vma=False,
    )
```

```python
import jax
import jax.numpy as jnp
from jax import lax
from jax.experimental import pallas as pl
from jax.experimental.pallas import tpu as pltpu
from jax.sharding import PartitionSpec as P

EPS = 1e-06
RATE = 8.0
AHEAD = 2
LANES = 128


def swap(value, axis):
    return lax.ppermute(value, axis, [(0, 1), (1, 0)])


def sigmoid(v):
    return 1.0 / (1.0 + jnp.exp(-v))


def rec_kernel(in_ref, gate_ref, conv_ref, map_ref, rate_ref, extra_ref, out_ref):
    length = in_ref.shape[0]
    taps = conv_ref.shape[0]
    values = in_ref[...].astype(jnp.float32)
    row = lax.broadcasted_iota(jnp.int32, values.shape, 0)
    conv = conv_ref[taps - 1 : taps, :] * values
    for back in range(1, taps):
        moved = jnp.where(row >= back, pltpu.roll(values, back, 0), 0.0)
        conv = conv + conv_ref[taps - 1 - back : taps - back, :] * moved
    mapped = jnp.dot(
        conv, map_ref[0], preferred_element_type=jnp.float32, precision=lax.Precision.HIGHEST
    )
    recur = sigmoid(mapped[:, :LANES])
    ingate = sigmoid(mapped[:, LANES:])
    log_rate = rate_ref[...] * recur - extra_ref[...]
    a = jnp.exp(log_rate)
    u = -2.0 * log_rate
    series = u * (1 - u / 2 * (1 - u / 3 * (1 - u / 4 * (1 - u / 5 * (1 - u / 6)))))
    b = jnp.sqrt(jnp.where(u < 0.25, series, 1.0 - jnp.exp(-u))) * (ingate * conv)
    inner = row % 8
    for s in (1, 2, 4):
        keep = inner >= s
        b = jnp.where(keep, a * pltpu.roll(b, s, 0) + b, b)
        a = jnp.where(keep, a * pltpu.roll(a, s, 0), a)
    s = 1
    groups = length // 8
    last_a = a.reshape(groups, 8, LANES)
    last_b = b.reshape(groups, 8, LANES)
    ca = jnp.broadcast_to(last_a[:, 7:8, :], last_a.shape).reshape(length, LANES)
    cb = jnp.broadcast_to(last_b[:, 7:8, :], last_b.shape).reshape(length, LANES)
    s = 8
    while s < length:
        cb_new = ca[s:] * cb[:-s] + cb[s:]
        ca_new = ca[s:] * ca[:-s]
        cb = jnp.concatenate([cb[:s], cb_new], axis=0)
        ca = jnp.concatenate([ca[:s], ca_new], axis=0)
        s *= 2
    state = jnp.concatenate([b[:8], a[8:] * cb[:-8] + b[8:]], axis=0)
    g = gate_ref[...].astype(jnp.float32)
    gelu = 0.5 * g * (1.0 + jnp.tanh(0.7978845608028654 * (g + 0.044715 * g * g * g)))
    out_ref[...] = (state * gelu).astype(out_ref.dtype)


def recurrence(branch_in, branch_gate, conv_weight, maps, rate, extra):
    length, width = branch_in.shape
    taps = conv_weight.shape[0]
    tile = lambda rows: pl.BlockSpec((rows, LANES), lambda i: (0, i))
    return pl.pallas_call(
        rec_kernel,
        grid=(width // LANES,),
        in_specs=[
            tile(length),
            tile(length),
            tile(taps),
            pl.BlockSpec((1, LANES, 2 * LANES), lambda i: (i, 0, 0)),
            tile(1),
            pl.BlockSpec((length, 1), lambda i: (0, 0)),
        ],
        out_specs=tile(length),
        out_shape=jax.ShapeDtypeStruct((length, width), jnp.bfloat16),
        cost_estimate=pl.CostEstimate(
            flops=length * width * 16000, bytes_accessed=length * width * 6, transcendentals=0
        ),
        name="recur",
    )(branch_in, branch_gate, conv_weight, maps, rate, extra)


def local(mesh_fs, *args):
    (
        tokens,
        mix_gain,
        lru_input,
        lru_gate,
        lru_input_scale,
        lru_gate_scale,
        conv_weight,
        recur_gate,
        input_gate,
        decay_rate,
        extra_decay,
        lru_output,
        lru_output_scale,
        ffn_gain,
        ffn_gate,
        ffn_up,
        ffn_gate_scale,
        ffn_up_scale,
        ffn_down,
        ffn_down_scale,
    ) = args
    ny = 2 if mesh_fs % 2 == 0 else 1
    nz = mesh_fs // ny
    fs = lax.axis_index("fs")
    z, y = fs // ny, fs % ny
    rep = lax.axis_index("rep")
    tp = lax.axis_index("tp")
    columns = tokens.shape[1]
    bf16, f32 = jnp.bfloat16, jnp.float32

    def half(v, axis):
        size = v.shape[axis] // 2
        return lax.dynamic_slice_in_dim(v, rep * size, size, axis)

    def ring(v, dz, dy):
        pairs = [
            (a * ny + b, ((a + dz) % nz) * ny + (b + dy) % ny)
            for a in range(nz)
            for b in range(ny)
        ]
        return lax.ppermute(v, "fs", pairs)

    chains = {}

    def send(v, dz, dy):
        chain = chains.setdefault((dz, dy), [])
        if len(chain) >= AHEAD:
            v, _ = lax.optimization_barrier((v, chain[-AHEAD]))
        got = ring(v, dz, dy)
        chain.append(got)
        return got

    def swap_y(parts):
        if ny == 1:
            return []
        return [(send(v, 0, 1), src_z, 1 - yy, at) for v, src_z, yy, at in parts]

    def direct_z(piece):
        return [
            (piece if dz == 0 else ring(piece, dz, 0), dz, 0, 0) for dz in range(nz)
        ]

    def tie(parts, after):
        values, _ = lax.optimization_barrier(([p[0] for p in parts], after))
        return [(v, *p[1:]) for v, p in zip(values, parts)]

    def place(parts, shape, axis):
        whole = jnp.zeros([n * (mesh_fs if i == axis else 1) for i, n in enumerate(shape)], bf16)
        for v, dz, yy, at in parts:
            src = ((z - dz + nz) % nz) * ny + (y + yy) % ny
            start = [0, 0]
            start[axis] = src * shape[axis]
            start[0] = start[0] + at
            whole = lax.dynamic_update_slice(whole, v, start)
        return whole

    def pair_piece(first, second):
        return jnp.concatenate([half(first, 1), half(second, 1)], axis=1).astype(bf16)

    other_half = swap(tokens, "tp")
    pair_tokens = swap(tokens, "rep")
    pair_other = swap(pair_tokens, "tp")
    pair_extra = swap(extra_decay, "rep")

    mix_piece = pair_piece(lru_input, lru_gate)
    out_piece = half(lru_output, 0).astype(bf16)
    down_piece = half(ffn_down, 0).astype(bf16)
    mix_parts = direct_z(mix_piece)
    mix_parts = mix_parts + swap_y(mix_parts)
    out_parts = direct_z(out_piece)
    mix_w = place(mix_parts, mix_piece.shape, 0)
    gate_w = lax.all_gather(half(ffn_gate, 1).astype(bf16), "fs", axis=0, tiled=True)
    up_w = lax.all_gather(half(ffn_up, 1).astype(bf16), "fs", axis=0, tiled=True)
    down_w = lax.all_gather(down_piece, "fs", axis=1, tiled=True)

    def finish(parts, piece, after):
        first = [(ring(parts[0][0], 0, 1), 0, 1, 0)] if ny > 1 else []
        rest = tie(parts[1:], after)
        crossed = [(ring(p[0], 0, 1), p[1], 1, 0) for p in rest] if ny > 1 else []
        return place(parts[:1] + rest + first + crossed, piece.shape, 1)

    def normed(own, other, gain):
        low = jnp.where(tp == 0, own, other).astype(f32)
        high = jnp.where(tp == 0, other, own).astype(f32)
        total = jnp.sum(low * low, axis=-1, keepdims=True) + jnp.sum(
            high * high, axis=-1, keepdims=True
        )
        scale = lax.rsqrt(total / (2 * columns) + EPS)
        return jnp.concatenate(
            [
                (low * scale * gain[:columns]).astype(bf16),
                (high * scale * gain[columns:]).astype(bf16),
            ],
            axis=1,
        )

    def dot(left, right):
        return jnp.dot(left, right, preferred_element_type=f32)

    nblocks, bdim = half(recur_gate, 0).shape[:2]
    per = LANES // bdim
    eye = jnp.eye(per, dtype=f32)

    def block_diag(blocks):
        grouped = half(blocks, 0).reshape(nblocks // per, per, bdim, bdim)
        return jnp.einsum("gpij,pq->gpiqj", grouped, eye, precision="highest").reshape(
            nblocks // per, LANES, LANES
        )

    maps = jnp.concatenate([block_diag(recur_gate), block_diag(input_gate)], axis=2)
    rate = (-RATE * jax.nn.softplus(-half(decay_rate, 0)))[None, :]
    taps = half(conv_weight, 1)
    mix_scale = jnp.concatenate([half(lru_input_scale, 0), half(lru_gate_scale, 0)])

    def branches_of(own, other):
        return (dot(normed(own, other, mix_gain), mix_w) * mix_scale).astype(bf16)

    def gated_of(branches, extra):
        width = branches.shape[1] // 2
        return recurrence(
            branches[:, :width], branches[:, width:], taps, maps, rate, extra[:, None]
        )

    def core_sum(terms):
        mine = lax.dynamic_slice_in_dim(terms, tp * columns, columns, 1)
        theirs = lax.dynamic_slice_in_dim(terms, (1 - tp) * columns, columns, 1).astype(bf16)
        return mine + swap(theirs, "tp").astype(f32)

    def own(v):
        return lax.dynamic_slice_in_dim(v, tp * columns, columns)

    pair_branches = branches_of(pair_tokens, pair_other)
    out_w = finish(out_parts, out_piece, pair_branches)
    pair_gated = gated_of(pair_branches, pair_extra)
    gated = gated_of(branches_of(tokens, other_half), extra_decay)
    sent = swap(core_sum(dot(pair_gated, out_w)).astype(bf16), "rep")
    total = core_sum(dot(gated, out_w)) + sent.astype(f32)
    mixed = (tokens.astype(f32) + total * own(lru_output_scale)).astype(bf16)

    mixed_other = swap(mixed, "tp")
    pair_mixed = swap(mixed, "rep")
    pair_mixed_other = swap(pair_mixed, "tp")

    def hidden_of(own_part, other_part):
        rows = normed(own_part, other_part, ffn_gain)
        gate = dot(rows, gate_w) * half(ffn_gate_scale, 0)
        return (jax.nn.silu(gate) * (dot(rows, up_w) * half(ffn_up_scale, 0))).astype(bf16)

    pair_hidden = hidden_of(pair_mixed, pair_mixed_other)
    hidden = hidden_of(mixed, mixed_other)
    cut = pair_hidden.shape[0] // 2
    summed = jnp.concatenate(
        [
            swap(core_sum(dot(pair_hidden[i : i + cut], down_w)).astype(bf16), "rep").astype(f32)
            for i in (0, cut)
        ]
    ) + core_sum(dot(hidden, down_w))
    return (mixed.astype(f32) + summed * own(ffn_down_scale)).astype(bf16)


def solution(mesh):
    in_specs = (
        P(("rep", "fs"), "tp"),
        P(),
        P("fs", "tp"),
        P("fs", "tp"),
        P("tp"),
        P("tp"),
        P(None, "tp"),
        P("tp", None, None),
        P("tp", None, None),
        P("tp"),
        P(("rep", "fs")),
        P("tp", "fs"),
        P(),
        P(),
        P("fs", "tp"),
        P("fs", "tp"),
        P("tp"),
        P("tp"),
        P("tp", "fs"),
        P(),
    )
    out_specs = P(("rep", "fs"), "tp")
    mesh_fs = mesh.shape["fs"]
    return jax.shard_map(
        lambda *args: local(mesh_fs, *args),
        mesh=mesh,
        in_specs=in_specs,
        out_specs=out_specs,
        check_vma=False,
    )
```

```python
import jax
import jax.numpy as jnp
from jax import lax
from jax.experimental import pallas as pl
from jax.experimental.pallas import tpu as pltpu
from jax.sharding import PartitionSpec as P

EPS = 1e-06
RATE = 8.0
AHEAD = 2
LANES = 128


def swap(value, axis):
    return lax.ppermute(value, axis, [(0, 1), (1, 0)])


def sigmoid(v):
    return 1.0 / (1.0 + jnp.exp(-v))


def rec_kernel(in_ref, gate_ref, conv_ref, map_ref, rate_ref, extra_ref, out_ref):
    length = in_ref.shape[0]
    taps = conv_ref.shape[0]
    values = in_ref[...].astype(jnp.float32)
    row = lax.broadcasted_iota(jnp.int32, values.shape, 0)
    conv = conv_ref[taps - 1 : taps, :] * values
    for back in range(1, taps):
        moved = jnp.where(row >= back, pltpu.roll(values, back, 0), 0.0)
        conv = conv + conv_ref[taps - 1 - back : taps - back, :] * moved
    mapped = jnp.dot(
        conv, map_ref[0], preferred_element_type=jnp.float32, precision=lax.Precision.HIGHEST
    )
    recur = sigmoid(mapped[:, :LANES])
    ingate = sigmoid(mapped[:, LANES:])
    log_rate = rate_ref[...] * recur - extra_ref[...]
    a = jnp.exp(log_rate)
    u = -2.0 * log_rate
    series = u * (1 - u / 2 * (1 - u / 3 * (1 - u / 4 * (1 - u / 5 * (1 - u / 6)))))
    b = jnp.sqrt(jnp.where(u < 0.25, series, 1.0 - jnp.exp(-u))) * (ingate * conv)
    inner = row % 8
    for s in (1, 2, 4):
        keep = inner >= s
        b = jnp.where(keep, a * pltpu.roll(b, s, 0) + b, b)
        a = jnp.where(keep, a * pltpu.roll(a, s, 0), a)
    s = 1
    groups = length // 8
    last_a = a.reshape(groups, 8, LANES)
    last_b = b.reshape(groups, 8, LANES)
    ca = jnp.broadcast_to(last_a[:, 7:8, :], last_a.shape).reshape(length, LANES)
    cb = jnp.broadcast_to(last_b[:, 7:8, :], last_b.shape).reshape(length, LANES)
    s = 8
    while s < length:
        cb_new = ca[s:] * cb[:-s] + cb[s:]
        ca_new = ca[s:] * ca[:-s]
        cb = jnp.concatenate([cb[:s], cb_new], axis=0)
        ca = jnp.concatenate([ca[:s], ca_new], axis=0)
        s *= 2
    state = jnp.concatenate([b[:8], a[8:] * cb[:-8] + b[8:]], axis=0)
    g = gate_ref[...].astype(jnp.float32)
    gelu = 0.5 * g * (1.0 + jnp.tanh(0.7978845608028654 * (g + 0.044715 * g * g * g)))
    out_ref[...] = (state * gelu).astype(out_ref.dtype)


def recurrence(branch_in, branch_gate, conv_weight, maps, rate, extra):
    length, width = branch_in.shape
    taps = conv_weight.shape[0]
    tile = lambda rows: pl.BlockSpec((rows, LANES), lambda i: (0, i))
    return pl.pallas_call(
        rec_kernel,
        grid=(width // LANES,),
        in_specs=[
            tile(length),
            tile(length),
            tile(taps),
            pl.BlockSpec((1, LANES, 2 * LANES), lambda i: (i, 0, 0)),
            tile(1),
            pl.BlockSpec((length, 1), lambda i: (0, 0)),
        ],
        out_specs=tile(length),
        out_shape=jax.ShapeDtypeStruct((length, width), jnp.bfloat16),
        cost_estimate=pl.CostEstimate(
            flops=length * width * 16000, bytes_accessed=length * width * 6, transcendentals=0
        ),
        name="recur",
    )(branch_in, branch_gate, conv_weight, maps, rate, extra)


def local(mesh_fs, *args):
    (
        tokens,
        mix_gain,
        lru_input,
        lru_gate,
        lru_input_scale,
        lru_gate_scale,
        conv_weight,
        recur_gate,
        input_gate,
        decay_rate,
        extra_decay,
        lru_output,
        lru_output_scale,
        ffn_gain,
        ffn_gate,
        ffn_up,
        ffn_gate_scale,
        ffn_up_scale,
        ffn_down,
        ffn_down_scale,
    ) = args
    ny = 2 if mesh_fs % 2 == 0 else 1
    nz = mesh_fs // ny
    fs = lax.axis_index("fs")
    z, y = fs // ny, fs % ny
    rep = lax.axis_index("rep")
    tp = lax.axis_index("tp")
    columns = tokens.shape[1]
    bf16, f32 = jnp.bfloat16, jnp.float32

    def half(v, axis):
        size = v.shape[axis] // 2
        return lax.dynamic_slice_in_dim(v, rep * size, size, axis)

    def ring(v, dz, dy):
        pairs = [
            (a * ny + b, ((a + dz) % nz) * ny + (b + dy) % ny)
            for a in range(nz)
            for b in range(ny)
        ]
        return lax.ppermute(v, "fs", pairs)

    chains = {}

    def send(v, dz, dy):
        chain = chains.setdefault((dz, dy), [])
        if len(chain) >= AHEAD:
            v, _ = lax.optimization_barrier((v, chain[-AHEAD]))
        got = ring(v, dz, dy)
        chain.append(got)
        return got

    def swap_y(parts):
        if ny == 1:
            return []
        return [(send(v, 0, 1), src_z, 1 - yy, at) for v, src_z, yy, at in parts]

    def direct_z(piece):
        return [
            (piece if dz == 0 else ring(piece, dz, 0), dz, 0, 0) for dz in range(nz)
        ]

    def tie(parts, after):
        values, _ = lax.optimization_barrier(([p[0] for p in parts], after))
        return [(v, *p[1:]) for v, p in zip(values, parts)]

    def place(parts, shape, axis):
        whole = jnp.zeros([n * (mesh_fs if i == axis else 1) for i, n in enumerate(shape)], bf16)
        for v, dz, yy, at in parts:
            src = ((z - dz + nz) % nz) * ny + (y + yy) % ny
            start = [0, 0]
            start[axis] = src * shape[axis]
            start[0] = start[0] + at
            whole = lax.dynamic_update_slice(whole, v, start)
        return whole

    def pair_piece(first, second):
        return jnp.concatenate([half(first, 1), half(second, 1)], axis=1).astype(bf16)

    other_half = swap(tokens, "tp")
    pair_tokens = swap(tokens, "rep")
    pair_other = swap(pair_tokens, "tp")
    pair_extra = swap(extra_decay, "rep")

    mix_piece = pair_piece(lru_input, lru_gate)
    out_piece = half(lru_output, 0).astype(bf16)
    down_piece = half(ffn_down, 0).astype(bf16)
    mix_parts = direct_z(mix_piece)
    mix_parts = mix_parts + swap_y(mix_parts)
    out_parts = direct_z(out_piece)
    mix_w = place(mix_parts, mix_piece.shape, 0)
    late = mix_parts[2 if nz > 2 else 0][0]

    def tied(value, after):
        return lax.optimization_barrier((value, after))[0]

    gate_w = lax.all_gather(
        tied(half(ffn_gate, 1).astype(bf16), late), "fs", axis=0, tiled=True
    )
    up_w = lax.all_gather(half(ffn_up, 1).astype(bf16), "fs", axis=0, tiled=True)

    def finish(parts, piece, after):
        first = [(ring(parts[0][0], 0, 1), 0, 1, 0)] if ny > 1 else []
        rest = tie(parts[1:], after)
        crossed = [(ring(p[0], 0, 1), p[1], 1, 0) for p in rest] if ny > 1 else []
        return place(parts[:1] + rest + first + crossed, piece.shape, 1)

    def normed(own, other, gain):
        low = jnp.where(tp == 0, own, other).astype(f32)
        high = jnp.where(tp == 0, other, own).astype(f32)
        total = jnp.sum(low * low, axis=-1, keepdims=True) + jnp.sum(
            high * high, axis=-1, keepdims=True
        )
        scale = lax.rsqrt(total / (2 * columns) + EPS)
        return jnp.concatenate(
            [
                (low * scale * gain[:columns]).astype(bf16),
                (high * scale * gain[columns:]).astype(bf16),
            ],
            axis=1,
        )

    def dot(left, right):
        return jnp.dot(left, right, preferred_element_type=f32)

    nblocks, bdim = half(recur_gate, 0).shape[:2]
    per = LANES // bdim
    eye = jnp.eye(per, dtype=f32)

    def block_diag(blocks):
        grouped = half(blocks, 0).reshape(nblocks // per, per, bdim, bdim)
        return jnp.einsum("gpij,pq->gpiqj", grouped, eye, precision="highest").reshape(
            nblocks // per, LANES, LANES
        )

    maps = jnp.concatenate([block_diag(recur_gate), block_diag(input_gate)], axis=2)
    rate = (-RATE * jax.nn.softplus(-half(decay_rate, 0)))[None, :]
    taps = half(conv_weight, 1)
    mix_scale = jnp.concatenate([half(lru_input_scale, 0), half(lru_gate_scale, 0)])

    def branches_of(own, other):
        return (dot(normed(own, other, mix_gain), mix_w) * mix_scale).astype(bf16)

    def gated_of(branches, extra):
        width = branches.shape[1] // 2
        return recurrence(
            branches[:, :width], branches[:, width:], taps, maps, rate, extra[:, None]
        )

    def core_sum(terms):
        mine = lax.dynamic_slice_in_dim(terms, tp * columns, columns, 1)
        theirs = lax.dynamic_slice_in_dim(terms, (1 - tp) * columns, columns, 1).astype(bf16)
        return mine + swap(theirs, "tp").astype(f32)

    def own(v):
        return lax.dynamic_slice_in_dim(v, tp * columns, columns)

    pair_branches = branches_of(pair_tokens, pair_other)
    down_parts = direct_z(tied(down_piece, pair_branches))
    pair_gated = gated_of(pair_branches, pair_extra)
    out_w = finish(out_parts, out_piece, pair_gated)
    pair_sum = core_sum(dot(pair_gated, out_w)).astype(bf16)
    sent = swap(pair_sum, "rep")
    gated = gated_of(tied(branches_of(tokens, other_half), pair_sum), extra_decay)
    down_w = finish(down_parts, down_piece, gated)
    total = core_sum(dot(gated, out_w)) + sent.astype(f32)
    mixed = (tokens.astype(f32) + total * own(lru_output_scale)).astype(bf16)

    mixed_other = swap(mixed, "tp")
    pair_mixed = swap(mixed, "rep")
    pair_mixed_other = swap(pair_mixed, "tp")

    def hidden_of(own_part, other_part):
        rows = normed(own_part, other_part, ffn_gain)
        gate = dot(rows, gate_w) * half(ffn_gate_scale, 0)
        return (jax.nn.silu(gate) * (dot(rows, up_w) * half(ffn_up_scale, 0))).astype(bf16)

    pair_hidden = hidden_of(pair_mixed, pair_mixed_other)
    hidden = hidden_of(mixed, mixed_other)
    sent = swap(core_sum(dot(pair_hidden, down_w)).astype(bf16), "rep")
    summed = core_sum(dot(hidden, down_w)) + sent.astype(f32)
    return (mixed.astype(f32) + summed * own(ffn_down_scale)).astype(bf16)


def solution(mesh):
    in_specs = (
        P(("rep", "fs"), "tp"),
        P(),
        P("fs", "tp"),
        P("fs", "tp"),
        P("tp"),
        P("tp"),
        P(None, "tp"),
        P("tp", None, None),
        P("tp", None, None),
        P("tp"),
        P(("rep", "fs")),
        P("tp", "fs"),
        P(),
        P(),
        P("fs", "tp"),
        P("fs", "tp"),
        P("tp"),
        P("tp"),
        P("tp", "fs"),
        P(),
    )
    out_specs = P(("rep", "fs"), "tp")
    mesh_fs = mesh.shape["fs"]
    return jax.shard_map(
        lambda *args: local(mesh_fs, *args),
        mesh=mesh,
        in_specs=in_specs,
        out_specs=out_specs,
        check_vma=False,
    )
```
